32 devices in a mesh: sp: 8 (over z, y), tp: 4 (over x, core).
Axes of the slice: x: 2, y: 2, z: 4, core: 2. Of those that a mesh axis runs over, the one named last changes fastest.
Arguments:
- tokens: bfloat16 [4096, 2048], P(('sp', 'tp')), may hold values from -8 to 8, as said below
- w_query: bfloat16 [2048, 1024], P(None, 'tp'), may hold values from -0.125 to 0.125
- w_key: bfloat16 [2048, 1024], P(None, 'tp'), may hold values from -0.125 to 0.125
- w_value: bfloat16 [2048, 1024], P(None, 'tp'), may hold values from -0.125 to 0.125
- head_bias: float32 [16], P('tp'), may hold values from -40 to -3
- w_out: bfloat16 [1024, 2048], P('tp'), may hold values from -0.1875 to 0.1875
Outputs:
- mixed: bfloat16 [4096, 2048], P(('sp', 'tp'))
The draws below stay inside these ranges and needn't reach their ends.
Inputs may be any that keep to these rules, and one draw needn't show every extreme that they name: `tokens`: activations of order one whose mean shifts between blocks of 512 positions.
All inputs are finite; a program needn't handle non-finite values.
Results may differ from the reference program's by a relative error of at most 0.014.
Values may be sent and summed in bfloat16 or wider, within the bound.
A program may use at most 128 MiB of HBM per device.

```python
import jax
import jax.numpy as jnp
from jax import lax

D = 2048
HEADS = 16
HEAD_DIM = 64
TOK_DEV = 512
TOKENS = 4096
N_SP = 8
N_TP = 4


def draw_tokens(key, part):
    noise = jax.random.normal(jax.random.fold_in(key, 11), (TOKENS, D), jnp.float32)
    spread_level = 1.0
    direction = jax.random.normal(jax.random.fold_in(key, 12), (D,), jnp.float32)
    region_scale = jax.random.uniform(jax.random.fold_in(key, 13), (TOKENS // TOK_DEV,), jnp.float32, -1.2, 1.2)
    level = jnp.repeat(region_scale, TOK_DEV) * spread_level
    values = 0.8 * noise + level[:, None] * direction[None, :]
    return jnp.clip(values, -8.0, 8.0).astype(jnp.bfloat16)


def draw_head_bias(key, part):
    fast_count = HEADS // 2
    ranking = jax.random.permutation(jax.random.fold_in(key, 21), HEADS)
    is_fast = ranking < fast_count
    slow_value = -jnp.log(jnp.float32(TOKENS)) - 1.0 + jax.random.uniform(jax.random.fold_in(key, 22), (HEADS,), jnp.float32, -0.5, 0.5)
    fast_value = -jnp.log(jax.random.uniform(jax.random.fold_in(key, 23), (HEADS,), jnp.float32, 30.0, 100.0)) - 1.0
    return jnp.where(is_fast, fast_value, slow_value).astype(jnp.float32)


def levels(stream_key, extent, split, smallest, largest):
    gain, own = 1.0, jax.random.fold_in(stream_key, 6)
    for dim, shards_of in split:
        draws = jnp.exp(jax.random.uniform(jax.random.fold_in(own, dim), (shards_of,), jnp.float32, smallest / len(split), largest / len(split)))
        gain = gain * jnp.repeat(draws, extent[dim] // shards_of).reshape([-1 if axis == dim else 1 for axis in range(len(extent))])
    return gain


def centred(key, dims, deviation, bound, shards=(), kind=jnp.bfloat16):
    values = deviation * jax.random.normal(key, dims, jnp.float32)
    if shards:
        values = values * levels(key, dims, shards, -0.22, 0.18)
    return jnp.clip(values, -bound, bound).astype(kind)


def setup_inputs(seed: int = 0) -> dict:
    key_of = jax.random.split(jax.random.key(seed), 7)
    tokens = draw_tokens(jax.random.fold_in(key_of[6], 71), 0)
    w_query = centred(key_of[1], (D, HEADS * HEAD_DIM), D ** -0.5, 0.125, ((1, 4),))
    w_key = centred(key_of[2], (D, HEADS * HEAD_DIM), D ** -0.5, 0.125, ((1, 4),))
    w_value = centred(key_of[3], (D, HEADS * HEAD_DIM), D ** -0.5, 0.125, ((1, 4),))
    head_bias = draw_head_bias(jax.random.fold_in(key_of[6], 71), 0)
    w_out = centred(key_of[5], (HEADS * HEAD_DIM, D), (HEADS * HEAD_DIM) ** -0.5, 0.1875, ((0, 4),))
    return dict(tokens=tokens, w_query=w_query, w_key=w_key, w_value=w_value, head_bias=head_bias, w_out=w_out)


def reference(tokens, w_query, w_key, w_value, head_bias, w_out):
    query_all = jnp.dot(tokens, w_query, preferred_element_type=jnp.float32).astype(jnp.bfloat16)
    key_all = jnp.dot(tokens, w_key, preferred_element_type=jnp.float32).astype(jnp.bfloat16)
    value_all = jnp.dot(tokens, w_value, preferred_element_type=jnp.float32).astype(jnp.bfloat16)
    key_pos = jnp.arange(TOKENS, dtype=jnp.int32).reshape(N_SP, TOK_DEV)

    def by_head(head_index):
        first_col = (head_index * HEAD_DIM).astype(jnp.int32)
        query_head = lax.dynamic_slice_in_dim(query_all, first_col, HEAD_DIM, 1)
        key_head = lax.dynamic_slice_in_dim(key_all, first_col, HEAD_DIM, 1)
        value_head = lax.dynamic_slice_in_dim(value_all, first_col, HEAD_DIM, 1)
        value_segments = value_head.reshape(N_SP, TOK_DEV, HEAD_DIM).astype(jnp.float32)
        bias_value = head_bias[head_index]

        def by_block(block_index):
            first_row = (block_index * TOK_DEV).astype(jnp.int32)
            query_block = lax.dynamic_slice_in_dim(query_head, first_row, TOK_DEV, 0)
            query_pos = first_row + jnp.arange(TOK_DEV, dtype=jnp.int32)
            scores = jnp.dot(query_block, key_head.T, preferred_element_type=jnp.float32)
            scores = scores.reshape(TOK_DEV, N_SP, TOK_DEV) * (HEAD_DIM ** -0.5) + bias_value
            causal = key_pos[None] < query_pos[:, None, None]
            log_keep = jnp.where(causal, jax.nn.log_sigmoid(-scores), 0.0)
            tail = lax.cumsum(log_keep, axis=2, reverse=True) - log_keep
            weights = jnp.where(causal, jnp.exp(jax.nn.log_sigmoid(scores) + tail), 0.0).astype(jnp.bfloat16)
            segment_out = jnp.einsum('qst,std->qsd', weights.astype(jnp.float32), value_segments)
            segment_total = jnp.sum(log_keep, axis=2)
            later = lax.cumsum(segment_total, axis=1, reverse=True) - segment_total
            return jnp.sum(jnp.exp(later)[..., None] * segment_out, axis=1)

        return lax.map(by_block, jnp.arange(N_SP, dtype=jnp.int32)).reshape(TOKENS, HEAD_DIM)

    heads_out = lax.map(by_head, jnp.arange(HEADS, dtype=jnp.int32))
    attended = jnp.transpose(heads_out, (1, 0, 2)).reshape(TOKENS, HEADS * HEAD_DIM).astype(jnp.bfloat16)
    group_width = HEADS * HEAD_DIM // N_TP
    total = jnp.zeros((TOKENS, D), jnp.float32)
    for group_index in range(N_TP):
        lower = group_index * group_width
        partial_value = jnp.dot(attended[:, lower:lower + group_width], w_out[lower:lower + group_width, :],
                          preferred_element_type=jnp.float32).astype(jnp.bfloat16)
        partial_value = lax.optimization_barrier(partial_value)
        total = total + partial_value.astype(jnp.float32)
    return total.astype(jnp.bfloat16)
```

```python
import functools
import math

import jax
import jax.numpy as jnp
from jax import lax
from jax.experimental import pallas as pl
from jax.experimental.pallas import tpu as pltpu
from jax.sharding import PartitionSpec as P

MESH = pl.DeviceIdType.MESH
LOG2E = math.log2(math.e)
CHUNK = 256


def attention_kernel(
    n_sp, n_tp, heads, piece, bias_ref, q_ref, kv_ref, out_ref,
    q_all, kv_all, packed, tri, send_sem, recv_sem, local_sem, back_send, back_recv
):
    me = lax.axis_index("sp")
    col = lax.axis_index("tp")
    share_count = n_sp // heads
    seg = kv_ref.shape[1]
    width = kv_ref.shape[2]
    half = width // 2
    rows = q_ref.shape[2] * 2
    pieces = rows // piece
    my_head = me // share_count
    my_share = lax.rem(me, share_count)

    barrier = pltpu.get_barrier_semaphore()
    total = n_sp * n_tp
    flat = me * n_tp + col

    def greet(step, carry):
        other = lax.rem(flat + step, total)
        pl.semaphore_signal(
            barrier, inc=1, device_id=(other // n_tp, lax.rem(other, n_tp)), device_id_type=MESH
        )
        return carry

    lax.fori_loop(1, total, greet, 0)

    key_id = lax.broadcasted_iota(jnp.int32, (CHUNK, CHUNK), 0)
    out_id = lax.broadcasted_iota(jnp.int32, (CHUNK, CHUNK), 1)
    tri[...] = jnp.where(key_id > out_id, 1.0, 0.0).astype(jnp.bfloat16)
    own = [
        pltpu.make_async_copy(kv_ref.at[my_head], kv_all.at[me], local_sem.at[0]),
        pltpu.make_async_copy(
            q_ref.at[my_head, lax.rem(my_share + me, share_count)], q_all.at[me], local_sem.at[1]
        ),
    ]
    for copy in own:
        copy.start()
    pl.semaphore_wait(barrier, total - 1)

    def outgoing(step):
        peer = lax.rem(me + step, n_sp)
        head = peer // share_count
        share = lax.rem(lax.rem(peer, share_count) + me, share_count)
        return (
            pltpu.make_async_remote_copy(
                src_ref=kv_ref.at[head], dst_ref=kv_all.at[me],
                send_sem=send_sem.at[0, step], recv_sem=recv_sem.at[0, me],
                device_id=(peer, col), device_id_type=MESH,
            ),
            pltpu.make_async_remote_copy(
                src_ref=q_ref.at[head, share], dst_ref=q_all.at[me],
                send_sem=send_sem.at[1, step], recv_sem=recv_sem.at[1, me],
                device_id=(peer, col), device_id_type=MESH,
            ),
        )

    for step in range(1, n_sp):
        for copy in outgoing(step):
            copy.start()
    for copy in own:
        copy.wait()

    bias = bias_ref[0] * LOG2E
    lane = lax.broadcasted_iota(jnp.int32, (rows // 2, width), 1)

    def chunk_terms(q, keys, offset, row_first, state, diagonal):
        acc, later = state
        scores = lax.dot_general(
            q, keys, (((1,), (1,)), ((), ())), preferred_element_type=jnp.float32
        )
        z = scores * LOG2E + bias
        log_take = jnp.minimum(z, 0.0) - jnp.log2(1.0 + jnp.exp2(-jnp.abs(z)))
        keep = log_take - z
        if diagonal:
            q_pos = row_first + lax.broadcasted_iota(jnp.int32, z.shape, 0)
            k_pos = offset + lax.broadcasted_iota(jnp.int32, z.shape, 1)
            live = k_pos < q_pos
            keep = jnp.where(live, keep, 0.0)
        keep16 = keep.astype(jnp.bfloat16)
        tail = jnp.dot(keep16, tri[...], preferred_element_type=jnp.float32)
        weight = jnp.exp2(log_take + tail + later)
        if diagonal:
            weight = jnp.where(live, weight, 0.0)
        acc = acc + jnp.dot(
            weight.astype(jnp.bfloat16), keys, preferred_element_type=jnp.float32
        )
        later = later + (tail[:, 0:1] + keep16[:, 0:1].astype(jnp.float32))
        return acc, later

    def back(block, index, first_row):
        owner = first_row // piece + index
        return pltpu.make_async_remote_copy(
            src_ref=packed.at[block, index], dst_ref=out_ref.at[col * heads + my_head],
            send_sem=back_send.at[block, index], recv_sem=back_recv.at[col * heads + my_head],
            device_id=(block, owner), device_id_type=MESH,
        )

    def visit(block, carry):
        @pl.when(block != me)
        def _():
            for part, dst in ((0, kv_all), (1, q_all)):
                pltpu.make_async_copy(dst.at[block], dst.at[block], recv_sem.at[part, block]).wait()

        pair = q_all[block]
        zero = jnp.zeros_like(pair)
        low = jnp.where(lane < half, pair, zero)
        high = pltpu.roll(pair.astype(jnp.float32), half, 1).astype(pair.dtype)
        high = jnp.where(lane < half, high, zero)
        q = jnp.concatenate([low, high], axis=0)
        first_row = lax.rem(my_share + block, share_count) * rows

        state = (jnp.zeros((rows, width), jnp.float32), jnp.zeros((rows, 1), jnp.float32))
        for index in reversed(range(seg // CHUNK)):
            keys = kv_all[block, pl.ds(index * CHUNK, CHUNK), :]
            state = chunk_terms(q, keys, index * CHUNK, first_row, state, True)

        def earlier(step, state):
            segment = block - 1 - step
            for index in reversed(range(seg // CHUNK)):
                keys = kv_all[segment, pl.ds(index * CHUNK, CHUNK), :]
                state = chunk_terms(q, keys, index * CHUNK, 0, state, False)
            return state

        acc, _ = lax.fori_loop(0, block, earlier, state)
        for index in range(pieces):
            top = acc[index * piece : index * piece + piece // 2]
            bottom = acc[index * piece + piece // 2 : (index + 1) * piece]
            lanes = lax.broadcasted_iota(jnp.int32, top.shape, 1)
            folded = jnp.where(lanes < half, pltpu.roll(top, half, 1), bottom)
            packed[block, index] = folded.astype(jnp.bfloat16)
            owner = first_row // piece + index
            here = jnp.logical_and(block == me, owner == col)

            @pl.when(here)
            def _():
                out_ref[col * heads + my_head] = folded.astype(jnp.bfloat16)

            @pl.when(jnp.logical_not(here))
            def _():
                back(block, index, first_row).start()

        return carry

    lax.fori_loop(0, n_sp, visit, 0)

    for step in range(1, n_sp):
        for copy in outgoing(step):
            copy.wait_send()

    def drain(block, carry):
        first_row = lax.rem(my_share + block, share_count) * rows
        for index in range(pieces):
            owner = first_row // piece + index

            @pl.when(jnp.logical_not(jnp.logical_and(block == me, owner == col)))
            def _():
                back(block, index, first_row).wait_send()

        return carry

    lax.fori_loop(0, n_sp, drain, 0)

    share = (col * piece) // rows
    source_share = lax.rem(share + n_sp * share_count - me, share_count)
    for source_col in range(n_tp):
        for head in range(heads):
            slot = source_col * heads + head
            source = head * share_count + source_share

            @pl.when(jnp.logical_not(jnp.logical_and(source == me, source_col == col)))
            def _():
                pltpu.make_async_copy(
                    out_ref.at[slot], out_ref.at[slot], back_recv.at[slot]
                ).wait()


def shards(tokens, w_query, w_key, w_value, head_bias, w_out):
    local_width = w_query.shape[1]
    heads = head_bias.shape[0]
    head_size = local_width // heads
    n_sp = lax.axis_size("sp")
    n_tp = lax.axis_size("tp")
    device_rows = tokens.shape[0]
    own_rows = device_rows * n_tp
    share_count = n_sp // heads
    rows = own_rows // share_count
    width = 2 * head_size
    me = lax.axis_index("sp")

    gathered = lax.all_gather(tokens, "tp", axis=0, tiled=True)
    w_full = lax.all_gather(w_out, "tp", axis=0, tiled=True)
    joined = jnp.concatenate([w_query, w_key, w_value], axis=1)
    projected = jnp.dot(gathered, joined, preferred_element_type=jnp.float32)
    queries = (projected[:, :local_width] * head_size ** (-0.5)).astype(jnp.bfloat16)
    pairs = projected[:, local_width:].astype(jnp.bfloat16)
    kv = pairs.reshape(own_rows, 2, heads, head_size).transpose(2, 0, 1, 3)
    kv = kv.reshape(heads, own_rows, width)
    q = queries.reshape(share_count, 2, rows // 2, heads, head_size).transpose(3, 0, 2, 1, 4)
    q = q.reshape(heads, share_count, rows // 2, width)
    bias = lax.dynamic_slice_in_dim(head_bias, me // share_count, 1, 0)

    pieces = rows // device_rows
    vmem = pl.BlockSpec(memory_space=pltpu.VMEM)
    attended = pl.pallas_call(
        functools.partial(attention_kernel, n_sp, n_tp, heads, device_rows),
        out_shape=jax.ShapeDtypeStruct((n_tp * heads, device_rows // 2, width), jnp.bfloat16),
        in_specs=[pl.BlockSpec(memory_space=pltpu.SMEM), vmem, vmem],
        out_specs=vmem,
        scratch_shapes=[
            pltpu.VMEM((n_sp, rows // 2, width), jnp.bfloat16),
            pltpu.VMEM((n_sp, own_rows, width), jnp.bfloat16),
            pltpu.VMEM((n_sp, pieces, device_rows // 2, width), jnp.bfloat16),
            pltpu.VMEM((CHUNK, CHUNK), jnp.bfloat16),
            pltpu.SemaphoreType.DMA((2, n_sp)),
            pltpu.SemaphoreType.DMA((2, n_sp)),
            pltpu.SemaphoreType.DMA((2,)),
            pltpu.SemaphoreType.DMA((n_sp, pieces)),
            pltpu.SemaphoreType.DMA((n_tp * heads,)),
        ],
        compiler_params=pltpu.CompilerParams(collective_id=0, has_side_effects=True),
        cost_estimate=pl.CostEstimate(
            flops=4 * rows * n_sp * own_rows * n_sp * width, bytes_accessed=2**22, transcendentals=0
        ),
        name="attend",
    )(bias, q, kv)
    attended = attended.reshape(n_tp * heads, device_rows // 2, 2, head_size)
    attended = attended.transpose(2, 1, 0, 3).reshape(device_rows, n_tp * local_width)
    return jnp.dot(attended, w_full, preferred_element_type=jnp.float32).astype(jnp.bfloat16)


def solution(mesh):
    placed = (
        P(("sp", "tp"), None),
        P(None, "tp"),
        P(None, "tp"),
        P(None, "tp"),
        P("tp"),
        P("tp", None),
    )
    return jax.shard_map(
        shards, mesh=mesh, in_specs=placed, out_specs=P(("sp", "tp"), None), check_vma=False
    )
```

```python
import functools
import math

import jax
import jax.numpy as jnp
from jax import lax
from jax.experimental import pallas as pl
from jax.experimental.pallas import tpu as pltpu
from jax.sharding import PartitionSpec as P

MESH = pl.DeviceIdType.MESH
LOG2E = math.log2(math.e)
CHUNK = 256
PARTS = 4
COLS = 512


def layer_kernel(
    n_sp, n_tp, heads, bias_ref, tokens_ref, wq_ref, wk_ref, wv_ref, wo_ref, out_ref,
    tok, wqkv, wfull, kv_own, q_own, q_all, kv_all, packed, att, att_rows, tri,
    load_sem, tok_send, tok_recv, wo_send, wo_recv, kv_send, kv_recv, q_send, q_recv,
    back_send, back_recv,
):
    me = lax.axis_index("sp")
    col = lax.axis_index("tp")
    share_count = n_sp // heads
    device_rows = PARTS * tokens_ref.shape[1]
    rows, width = kv_own.shape[2], kv_own.shape[3]
    half = width // 2
    piece = min(rows, device_rows)
    pieces = rows // piece
    subs = device_rows // piece
    chunk_shares = CHUNK // rows
    seg_chunks = share_count * rows // CHUNK
    my_head = me // share_count
    my_share = lax.rem(me, share_count)
    core = lax.rem(col, 2)
    place = col // 2
    places = n_tp // 2
    sibling = place * 2 + 1 - core

    loads = [
        pltpu.make_async_copy(src, dst, load_sem.at[index])
        for index, (src, dst) in enumerate(
            [
                (tokens_ref, tok.at[col]),
                (wq_ref, wqkv.at[0]),
                (wk_ref, wqkv.at[1]),
                (wv_ref, wqkv.at[2]),
                (wo_ref, wfull.at[col]),
            ]
        )
    ]
    for copy in loads:
        copy.start()

    barrier = pltpu.get_barrier_semaphore()
    total = n_sp * n_tp
    flat = me * n_tp + col

    def greet(step, carry):
        other = lax.rem(flat + step, total)
        pl.semaphore_signal(
            barrier, inc=1, device_id=(other // n_tp, lax.rem(other, n_tp)), device_id_type=MESH
        )
        return carry

    lax.fori_loop(1, total, greet, 0)
    key_id = lax.broadcasted_iota(jnp.int32, (CHUNK, CHUNK), 0)
    out_id = lax.broadcasted_iota(jnp.int32, (CHUNK, CHUNK), 1)
    tri[...] = jnp.where(key_id > out_id, 1.0, 0.0).astype(jnp.bfloat16)
    pl.semaphore_wait(barrier, total - 1)

    def same_core(k):
        return lax.rem(place + k, places) * 2 + core

    def arrived(ref, sem):
        pltpu.make_async_copy(ref, ref, sem).wait()

    def token_copy(kind, part):
        if kind < places:
            src, block = tokens_ref.at[part], col
            target = sibling if kind == 0 else same_core(kind)
        else:
            block = same_core(kind - places + 1)
            src, target = tok.at[block, part], sibling
        return pltpu.make_async_remote_copy(
            src_ref=src, dst_ref=tok.at[block, part],
            send_sem=tok_send.at[kind, part], recv_sem=tok_recv.at[block, part],
            device_id=(me, target), device_id_type=MESH,
        )

    def wo_copy(kind):
        if kind < places:
            src, block = wo_ref, col
            target = sibling if kind == 0 else same_core(kind)
        else:
            block = same_core(kind - places + 1)
            src, target = wfull.at[block], sibling
        return pltpu.make_async_remote_copy(
            src_ref=src, dst_ref=wfull.at[block],
            send_sem=wo_send.at[kind], recv_sem=wo_recv.at[block],
            device_id=(me, target), device_id_type=MESH,
        )

    for part in range(PARTS):
        for kind in range(places):
            token_copy(kind, part).start()

    lane = lax.broadcasted_iota(jnp.int32, (rows, width), 1)
    lane_half = lax.broadcasted_iota(jnp.int32, (rows // 2, width), 1)

    def turn(value):
        return pltpu.roll(value, half, 1)

    def kv_copy(step, share):
        peer = lax.rem(me + step, n_sp)
        return pltpu.make_async_remote_copy(
            src_ref=kv_own.at[peer // share_count, share], dst_ref=kv_all.at[me, share],
            send_sem=kv_send.at[step, share], recv_sem=kv_recv.at[me, share],
            device_id=(peer, col), device_id_type=MESH,
        )

    def share_of(peer):
        return lax.rem(lax.rem(peer, share_count) + me, share_count)

    def q_copy(step):
        peer = lax.rem(me + step, n_sp)
        return pltpu.make_async_remote_copy(
            src_ref=q_own.at[peer // share_count, share_of(peer)], dst_ref=q_all.at[me],
            send_sem=q_send.at[step], recv_sem=q_recv.at[me],
            device_id=(peer, col), device_id_type=MESH,
        )

    def project(group):
        x = tok[pl.ds(group * pieces, pieces)].reshape(subs * rows, tok.shape[3])
        qf = jnp.dot(x, wqkv[0], preferred_element_type=jnp.float32) * half ** (-0.5)
        kf = jnp.dot(x, wqkv[1], preferred_element_type=jnp.float32)
        vf = jnp.dot(x, wqkv[2], preferred_element_type=jnp.float32)
        for sub in range(subs):
            own = slice(sub * rows, (sub + 1) * rows)
            publish(group * subs + sub, qf[own], kf[own], vf[own])

    def publish(share, qf, kf, vf):
        for pair in range(heads // 2):
            cols = slice(pair * width, (pair + 1) * width)
            kk, vv = kf[:, cols], vf[:, cols]
            top, low = qf[: rows // 2, cols], qf[rows // 2 :, cols]
            kv_own[2 * pair, share] = jnp.where(lane < half, kk, turn(vv)).astype(jnp.bfloat16)
            kv_own[2 * pair + 1, share] = jnp.where(lane < half, turn(kk), vv).astype(jnp.bfloat16)
            q_own[2 * pair, share] = jnp.where(lane_half < half, top, turn(low)).astype(
                jnp.bfloat16
            )
            q_own[2 * pair + 1, share] = jnp.where(lane_half < half, turn(top), low).astype(
                jnp.bfloat16
            )
        for step in range(1, n_sp):
            kv_copy(step, share).start()

            @pl.when(share_of(lax.rem(me + step, n_sp)) == share)
            def _():
                q_copy(step).start()

        kv_all[me, share] = kv_own[my_head, share]

        @pl.when(share_of(me) == share)
        def _():
            q_all[me] = q_own[my_head, share]

    for copy in loads:
        copy.wait()
    own_group = col // pieces
    groups = n_tp // pieces
    if pieces > 1:
        for part in range(PARTS):
            arrived(tok.at[sibling, part], tok_recv.at[sibling, part])
        project(own_group)
    for part in range(PARTS):
        for k in range(1, places):
            block = same_core(k)
            arrived(tok.at[block, part], tok_recv.at[block, part])
            token_copy(places + k - 1, part).start()
    for kind in range(places):
        wo_copy(kind).start()
    for part in range(PARTS):
        if pieces == 1:
            arrived(tok.at[sibling, part], tok_recv.at[sibling, part])
        for k in range(1, places):
            block = lax.rem(place + k, places) * 2 + 1 - core
            arrived(tok.at[block, part], tok_recv.at[block, part])

    def project_next(step, carry):
        project(lax.rem(own_group + step, groups))
        return carry

    lax.fori_loop(1 if pieces > 1 else 0, groups, project_next, 0)

    bias = bias_ref[my_head] * LOG2E

    def logs(q, keys):
        scores = lax.dot_general(
            q, keys, (((1,), (1,)), ((), ())), preferred_element_type=jnp.float32
        )
        z = scores * LOG2E + bias
        log_take = jnp.minimum(z, 0.0) - jnp.log2(1.0 + jnp.exp2(-jnp.abs(z)))
        return log_take, log_take - z

    def tails(keep):
        keep = keep.astype(jnp.bfloat16)
        tail = jnp.dot(keep, tri[...], preferred_element_type=jnp.float32)
        return tail, tail[:, 0:1] + keep[:, 0:1].astype(jnp.float32)

    def chunk_keys(index):
        block, inner = index // seg_chunks, lax.rem(index, seg_chunks)
        return kv_all[block, pl.ds(inner * chunk_shares, chunk_shares)].reshape(CHUNK, width)

    def weigh(log_take, tail, later, keys):
        weight = jnp.exp2(log_take + (tail + later)).astype(jnp.bfloat16)
        return jnp.dot(weight, keys, preferred_element_type=jnp.float32)

    def landing(first_row):
        return (col * heads + my_head) * subs + lax.rem(first_row // piece, subs)

    def is_here(block, index, first_row):
        return jnp.logical_and(block == me, (first_row + index * piece) // device_rows == col)

    def back(block, index, first_row):
        owner = (first_row + index * piece) // device_rows
        slot = landing(first_row)
        return pltpu.make_async_remote_copy(
            src_ref=packed.at[block, index], dst_ref=att.at[slot],
            send_sem=back_send.at[block, index], recv_sem=back_recv.at[slot],
            device_id=(block, owner), device_id_type=MESH,
        )

    def visit(block, carry):
        @pl.when(block != me)
        def _():
            for share in range(share_count):
                arrived(kv_all.at[block, share], kv_recv.at[block, share])
            arrived(q_all.at[block], q_recv.at[block])

        @pl.when(block == n_sp - 2)
        def _():
            for k in range(1, places):
                arrived(wfull.at[same_core(k)], wo_recv.at[same_core(k)])
                wo_copy(places + k - 1).start()

        pair = q_all[block].astype(jnp.float32)
        low = jnp.where(lane_half < half, pair, 0.0)
        high = jnp.where(lane_half < half, turn(pair), 0.0)
        q = jnp.concatenate([low, high], axis=0).astype(jnp.bfloat16)
        first_row = lax.rem(my_share + block, share_count) * rows
        diagonal = first_row // CHUNK
        q_pos = first_row + lax.broadcasted_iota(jnp.int32, (rows, CHUNK), 0)
        k_pos = diagonal * CHUNK + lax.broadcasted_iota(jnp.int32, (rows, CHUNK), 1)
        live = k_pos < q_pos

        keys = chunk_keys(block * seg_chunks + diagonal)
        log_take, keep = logs(q, keys)
        tail, later = tails(jnp.where(live, keep, 0.0))
        weight = jnp.where(live, jnp.exp2(log_take + tail), 0.0).astype(jnp.bfloat16)
        acc = jnp.dot(weight, keys, preferred_element_type=jnp.float32)

        def single(step, state):
            acc, later = state
            keys = chunk_keys(block * seg_chunks + diagonal - 1 - step)
            log_take, keep = logs(q, keys)
            tail, whole = tails(keep)
            return acc + weigh(log_take, tail, later, keys), later + whole

        def segment(step, state):
            acc, later = state
            first = (block - 1 - step) * seg_chunks
            keys = [chunk_keys(first + index) for index in reversed(range(seg_chunks))]
            terms = [logs(q, part) for part in keys]
            ends = [tails(keep) for _, keep in terms]
            for part, (log_take, _), (tail, whole) in zip(keys, terms, ends):
                acc = acc + weigh(log_take, tail, later, part)
                later = later + whole
            return acc, later

        state = lax.fori_loop(0, diagonal, single, (acc, later))
        acc, _ = lax.fori_loop(0, block, segment, state)
        for index in range(pieces):
            top = acc[index * piece : index * piece + piece // 2]
            low = acc[index * piece + piece // 2 : (index + 1) * piece]
            lanes = lax.broadcasted_iota(jnp.int32, top.shape, 1)
            folded = jnp.where(lanes < half, turn(top), low).astype(jnp.bfloat16)
            packed[block, index] = folded
            here = is_here(block, index, first_row)

            @pl.when(here)
            def _():
                att[landing(first_row)] = folded

            @pl.when(jnp.logical_not(here))
            def _():
                back(block, index, first_row).start()

        return carry

    lax.fori_loop(0, n_sp, visit, 0)

    for sub in range(subs):
        share = (col * device_rows + sub * piece) // rows
        source_share = lax.rem(share + n_sp * share_count - me, share_count)
        for source_col in range(n_tp):
            for pair in range(heads // 2):
                values = []
                for head in (2 * pair, 2 * pair + 1):
                    slot = (source_col * heads + head) * subs + sub
                    source = head * share_count + source_share

                    @pl.when(jnp.logical_not(jnp.logical_and(source == me, source_col == col)))
                    def _():
                        arrived(att.at[slot], back_recv.at[slot])

                    values.append(att[slot].astype(jnp.float32))
                lanes = lax.broadcasted_iota(jnp.int32, values[0].shape, 1)
                top = jnp.where(lanes < half, values[0], turn(values[1]))
                low = jnp.where(lanes < half, turn(values[0]), values[1])
                start = (source_col * heads + 2 * pair) * half
                cols = slice(start, start + width)
                middle = sub * piece + piece // 2
                att_rows[sub * piece : middle, cols] = top.astype(jnp.bfloat16)
                att_rows[middle : (sub + 1) * piece, cols] = low.astype(jnp.bfloat16)

    arrived(wfull.at[sibling], wo_recv.at[sibling])
    for k in range(1, places):
        block = lax.rem(place + k, places) * 2 + 1 - core
        arrived(wfull.at[block], wo_recv.at[block])
    for first in range(0, out_ref.shape[1], COLS):
        w = wfull[:, :, first : first + COLS].reshape(att_rows.shape[1], COLS)
        out_ref[:, first : first + COLS] = jnp.dot(
            att_rows[...], w, preferred_element_type=jnp.float32
        ).astype(jnp.bfloat16)

    for kind in range(2 * places - 1):
        wo_copy(kind).wait_send()
        for part in range(PARTS):
            token_copy(kind, part).wait_send()
    for step in range(1, n_sp):
        q_copy(step).wait_send()
        for share in range(share_count):
            kv_copy(step, share).wait_send()

    def drain(block, carry):
        first_row = lax.rem(my_share + block, share_count) * rows
        for index in range(pieces):
            here = is_here(block, index, first_row)

            @pl.when(jnp.logical_not(here))
            def _():
                back(block, index, first_row).wait_send()

        return carry

    lax.fori_loop(0, n_sp, drain, 0)


def shards(tokens, w_query, w_key, w_value, head_bias, w_out):
    model, local_width = w_query.shape
    heads = head_bias.shape[0]
    width = 2 * (local_width // heads)
    n_sp = lax.axis_size("sp")
    n_tp = lax.axis_size("tp")
    device_rows = tokens.shape[0]
    share_count = n_sp // heads
    rows = device_rows * n_tp // share_count
    piece = min(rows, device_rows)
    pieces = rows // piece
    slots = n_tp * heads * device_rows // piece
    out_width = w_out.shape[1]
    places = n_tp // 2
    kinds = 2 * places - 1

    smem = pl.BlockSpec(memory_space=pltpu.SMEM)
    anywhere = pl.BlockSpec(memory_space=pl.ANY)
    dma = pltpu.SemaphoreType.DMA

    def vmem(*shape):
        return pltpu.VMEM(shape, jnp.bfloat16)

    return pl.pallas_call(
        functools.partial(layer_kernel, n_sp, n_tp, heads),
        out_shape=jax.ShapeDtypeStruct((device_rows, out_width), jnp.bfloat16),
        in_specs=[smem] + [anywhere] * 5,
        out_specs=pl.BlockSpec(memory_space=pltpu.VMEM),
        scratch_shapes=[
            vmem(n_tp, PARTS, device_rows // PARTS, model),
            vmem(3, model, local_width),
            vmem(n_tp, local_width, out_width),
            vmem(heads, share_count, rows, width),
            vmem(heads, share_count, rows // 2, width),
            vmem(n_sp, rows // 2, width),
            vmem(n_sp, share_count, rows, width),
            vmem(n_sp, pieces, piece // 2, width),
            vmem(slots, piece // 2, width),
            vmem(device_rows, n_tp * local_width),
            vmem(CHUNK, CHUNK),
            dma((5,)),
            dma((kinds, PARTS)),
            dma((n_tp, PARTS)),
            dma((kinds,)),
            dma((n_tp,)),
            dma((n_sp, share_count)),
            dma((n_sp, share_count)),
            dma((n_sp,)),
            dma((n_sp,)),
            dma((n_sp, pieces)),
            dma((slots,)),
        ],
        compiler_params=pltpu.CompilerParams(
            collective_id=0, has_side_effects=True, vmem_limit_bytes=60 * 2**20
        ),
        name="layer",
    )(
        head_bias,
        tokens.reshape(PARTS, device_rows // PARTS, model),
        w_query, w_key, w_value, w_out,
    )


def solution(mesh):
    placed = (
        P(("sp", "tp"), None),
        P(None, "tp"),
        P(None, "tp"),
        P(None, "tp"),
        P("tp"),
        P("tp", None),
    )
    return jax.shard_map(
        shards, mesh=mesh, in_specs=placed, out_specs=P(("sp", "tp"), None), check_vma=False
    )
```

```python
import functools
import math

import jax
import jax.numpy as jnp
from jax import lax
from jax.experimental import pallas as pl
from jax.experimental.pallas import tpu as pltpu
from jax.sharding import PartitionSpec as P

MESH = pl.DeviceIdType.MESH
LOG2E = math.log2(math.e)
CHUNK = 256
PARTS = 4
COLS = 512
LOOK = 4
LOG_MAX = 126.0


def layer_kernel(
    n_sp, n_tp, heads, bias_ref, tokens_ref, wq_ref, wk_ref, wv_ref, wo_ref, out_ref,
    tok, wqkv, wfull, kv_own, q_own, q_all, kv_all, packed, att, att_rows, tri,
    load_sem, tok_send, tok_recv, wo_send, wo_recv, kv_send, pass_send, kv_recv, q_send, q_recv,
    back_send, back_recv,
):
    me = lax.axis_index("sp")
    col = lax.axis_index("tp")
    share_count = n_sp // heads
    device_rows = PARTS * tokens_ref.shape[1]
    rows, width = kv_own.shape[2], kv_own.shape[3]
    half = width // 2
    piece = min(rows, device_rows)
    pieces = rows // piece
    subs = device_rows // piece
    chunk_shares = CHUNK // rows
    seg_chunks = share_count * rows // CHUNK
    my_head = me // share_count
    my_share = lax.rem(me, share_count)
    core = lax.rem(col, 2)
    place = col // 2
    places = n_tp // 2
    sibling = place * 2 + 1 - core

    loads = [
        pltpu.make_async_copy(src, dst, load_sem.at[index])
        for index, (src, dst) in enumerate(
            [
                (tokens_ref, tok.at[col]),
                (wq_ref, wqkv.at[0]),
                (wk_ref, wqkv.at[1]),
                (wv_ref, wqkv.at[2]),
                (wo_ref, wfull.at[col]),
            ]
        )
    ]
    for copy in loads:
        copy.start()

    barrier = pltpu.get_barrier_semaphore()
    total = n_sp * n_tp
    flat = me * n_tp + col

    def greet(step, carry):
        other = lax.rem(flat + step, total)
        pl.semaphore_signal(
            barrier, inc=1, device_id=(other // n_tp, lax.rem(other, n_tp)), device_id_type=MESH
        )
        return carry

    lax.fori_loop(1, total, greet, 0)
    key_id = lax.broadcasted_iota(jnp.int32, (CHUNK, CHUNK), 0)
    out_id = lax.broadcasted_iota(jnp.int32, (CHUNK, CHUNK), 1)
    tri[...] = jnp.where(key_id > out_id, 1.0, 0.0).astype(jnp.bfloat16)
    pl.semaphore_wait(barrier, total - 1)

    def same_core(k):
        return lax.rem(place + k, places) * 2 + core

    def arrived(ref, sem):
        pltpu.make_async_copy(ref, ref, sem).wait()

    def token_copy(kind, part):
        if kind < places:
            src, block = tokens_ref.at[part], col
            target = sibling if kind == 0 else same_core(kind)
        else:
            block = same_core(kind - places + 1)
            src, target = tok.at[block, part], sibling
        return pltpu.make_async_remote_copy(
            src_ref=src, dst_ref=tok.at[block, part],
            send_sem=tok_send.at[kind, part], recv_sem=tok_recv.at[block, part],
            device_id=(me, target), device_id_type=MESH,
        )

    def wo_copy(kind):
        if kind < places:
            src, block = wo_ref, col
            target = sibling if kind == 0 else same_core(kind)
        else:
            block = same_core(kind - places + 1)
            src, target = wfull.at[block], sibling
        return pltpu.make_async_remote_copy(
            src_ref=src, dst_ref=wfull.at[block],
            send_sem=wo_send.at[kind], recv_sem=wo_recv.at[block],
            device_id=(me, target), device_id_type=MESH,
        )

    for part in range(PARTS):
        for kind in range(places):
            token_copy(kind, part).start()

    lane = lax.broadcasted_iota(jnp.int32, (rows, width), 1)
    lane_half = lax.broadcasted_iota(jnp.int32, (rows // 2, width), 1)

    def turn(value):
        return pltpu.roll(value, half, 1)

    def kv_copy(step, share):
        head = lax.rem(my_head + step, heads)
        return pltpu.make_async_remote_copy(
            src_ref=kv_own.at[head, share], dst_ref=kv_all.at[me, share],
            send_sem=kv_send.at[step, share], recv_sem=kv_recv.at[me, share],
            device_id=(head * share_count + my_share, col), device_id_type=MESH,
        )

    def forward(turn_of, step, share):
        block = turn_of * share_count + my_share
        peer = my_head * share_count + lax.rem(my_share + step, share_count)
        return pltpu.make_async_remote_copy(
            src_ref=kv_all.at[block, share], dst_ref=kv_all.at[block, share],
            send_sem=pass_send.at[turn_of, step, share], recv_sem=kv_recv.at[block, share],
            device_id=(peer, col), device_id_type=MESH,
        )

    def relay(block):
        for share in range(share_count):
            arrived(kv_all.at[block, share], kv_recv.at[block, share])
            for step in range(1, share_count):
                forward(block // share_count, step, share).start()

    def share_of(peer):
        return lax.rem(lax.rem(peer, share_count) + me, share_count)

    def q_copy(step):
        peer = lax.rem(me + step, n_sp)
        return pltpu.make_async_remote_copy(
            src_ref=q_own.at[peer // share_count, share_of(peer)], dst_ref=q_all.at[me],
            send_sem=q_send.at[step], recv_sem=q_recv.at[me],
            device_id=(peer, col), device_id_type=MESH,
        )

    def project(group):
        x = tok[pl.ds(group * pieces, pieces)].reshape(subs * rows, tok.shape[3])
        qf = jnp.dot(x, wqkv[0], preferred_element_type=jnp.float32) * (LOG2E * half ** (-0.5))
        kf = jnp.dot(x, wqkv[1], preferred_element_type=jnp.float32)
        vf = jnp.dot(x, wqkv[2], preferred_element_type=jnp.float32)
        for sub in range(subs):
            own = slice(sub * rows, (sub + 1) * rows)
            publish(group * subs + sub, qf[own], kf[own], vf[own])

    def publish(share, qf, kf, vf):
        for pair in range(heads // 2):
            cols = slice(pair * width, (pair + 1) * width)
            kk, vv = kf[:, cols], vf[:, cols]
            top, low = qf[: rows // 2, cols], qf[rows // 2 :, cols]
            kv_own[2 * pair, share] = jnp.where(lane < half, kk, turn(vv)).astype(jnp.bfloat16)
            kv_own[2 * pair + 1, share] = jnp.where(lane < half, turn(kk), vv).astype(jnp.bfloat16)
            q_own[2 * pair, share] = jnp.where(lane_half < half, top, turn(low)).astype(
                jnp.bfloat16
            )
            q_own[2 * pair + 1, share] = jnp.where(lane_half < half, turn(top), low).astype(
                jnp.bfloat16
            )
        for step in range(1, heads):
            kv_copy(step, share).start()
        kv_all[me, share] = kv_own[my_head, share]
        for step in range(1, share_count):
            forward(my_head, step, share).start()
        for step in range(1, n_sp):

            @pl.when(share_of(lax.rem(me + step, n_sp)) == share)
            def _():
                q_copy(step).start()

        @pl.when(share_of(me) == share)
        def _():
            q_all[me] = q_own[my_head, share]

    for copy in loads:
        copy.wait()
    own_group = col // pieces
    groups = n_tp // pieces
    if pieces > 1:
        for part in range(PARTS):
            arrived(tok.at[sibling, part], tok_recv.at[sibling, part])
        project(own_group)
    for part in range(PARTS):
        for k in range(1, places):
            block = same_core(k)
            arrived(tok.at[block, part], tok_recv.at[block, part])
            token_copy(places + k - 1, part).start()
    for kind in range(places):
        wo_copy(kind).start()
    for part in range(PARTS):
        if pieces == 1:
            arrived(tok.at[sibling, part], tok_recv.at[sibling, part])
        for k in range(1, places):
            block = lax.rem(place + k, places) * 2 + 1 - core
            arrived(tok.at[block, part], tok_recv.at[block, part])

    def project_next(step, carry):
        project(lax.rem(own_group + step, groups))
        return carry

    lax.fori_loop(1 if pieces > 1 else 0, groups, project_next, 0)

    bias = bias_ref[my_head] * LOG2E

    def logs(q, keys):
        scores = lax.dot_general(
            q, keys, (((1,), (1,)), ((), ())), preferred_element_type=jnp.float32
        )
        z = scores + bias
        lose = jnp.maximum(
            jnp.log(1.0 + jnp.exp2(jnp.minimum(z, LOG_MAX))) * LOG2E, z
        )
        return z - lose, lose

    def tails(lose):
        lose = lose.astype(jnp.bfloat16)
        tail = jnp.dot(lose, tri[...], preferred_element_type=jnp.float32)
        return tail, tail[:, 0:1] + lose[:, 0:1].astype(jnp.float32)

    def chunk_keys(index):
        block, inner = index // seg_chunks, lax.rem(index, seg_chunks)
        return kv_all[block, pl.ds(inner * chunk_shares, chunk_shares)].reshape(CHUNK, width)

    def weigh(log_take, tail, later, keys):
        weight = jnp.exp2(log_take - tail).astype(jnp.bfloat16)
        return jnp.exp2(-later) * jnp.dot(weight, keys, preferred_element_type=jnp.float32)

    def landing(first_row):
        return (col * heads + my_head) * subs + lax.rem(first_row // piece, subs)

    def is_here(block, index, first_row):
        return jnp.logical_and(block == me, (first_row + index * piece) // device_rows == col)

    def back(block, index, first_row):
        owner = (first_row + index * piece) // device_rows
        slot = landing(first_row)
        return pltpu.make_async_remote_copy(
            src_ref=packed.at[block, index], dst_ref=att.at[slot],
            send_sem=back_send.at[block, index], recv_sem=back_recv.at[slot],
            device_id=(block, owner), device_id_type=MESH,
        )

    def relayed(block):
        return jnp.logical_and(lax.rem(block, share_count) == my_share, block != me)

    for block in range(LOOK):

        @pl.when(relayed(block))
        def _():
            relay(block)

    def visit(block, carry):
        ahead = block + LOOK

        @pl.when(jnp.logical_and(ahead < n_sp, relayed(ahead)))
        def _():
            relay(ahead)

        @pl.when(lax.rem(block, share_count) != my_share)
        def _():
            for share in range(share_count):
                arrived(kv_all.at[block, share], kv_recv.at[block, share])

        @pl.when(block != me)
        def _():
            arrived(q_all.at[block], q_recv.at[block])

        @pl.when(block == n_sp - 2)
        def _():
            for k in range(1, places):
                arrived(wfull.at[same_core(k)], wo_recv.at[same_core(k)])
                wo_copy(places + k - 1).start()

        pair = q_all[block].astype(jnp.float32)
        low = jnp.where(lane_half < half, pair, 0.0)
        high = jnp.where(lane_half < half, turn(pair), 0.0)
        q = jnp.concatenate([low, high], axis=0).astype(jnp.bfloat16)
        first_row = lax.rem(my_share + block, share_count) * rows
        diagonal = first_row // CHUNK
        q_pos = first_row + lax.broadcasted_iota(jnp.int32, (rows, CHUNK), 0)
        k_pos = diagonal * CHUNK + lax.broadcasted_iota(jnp.int32, (rows, CHUNK), 1)
        live = k_pos < q_pos

        keys = chunk_keys(block * seg_chunks + diagonal)
        log_take, keep = logs(q, keys)
        tail, later = tails(jnp.where(live, keep, 0.0))
        weight = jnp.where(live, jnp.exp2(log_take - tail), 0.0).astype(jnp.bfloat16)
        acc = jnp.dot(weight, keys, preferred_element_type=jnp.float32)

        def single(step, state):
            acc, later = state
            keys = chunk_keys(block * seg_chunks + diagonal - 1 - step)
            log_take, keep = logs(q, keys)
            tail, whole = tails(keep)
            return acc + weigh(log_take, tail, later, keys), later + whole

        def segment(step, state):
            acc, later = state
            first = (block - 1 - step) * seg_chunks
            keys = [chunk_keys(first + index) for index in reversed(range(seg_chunks))]
            terms = [logs(q, part) for part in keys]
            ends = [tails(keep) for _, keep in terms]
            for part, (log_take, _), (tail, whole) in zip(keys, terms, ends):
                acc = acc + weigh(log_take, tail, later, part)
                later = later + whole
            return acc, later

        state = lax.fori_loop(0, diagonal, single, (acc, later))
        acc, _ = lax.fori_loop(0, block, segment, state)
        for index in range(pieces):
            top = acc[index * piece : index * piece + piece // 2]
            low = acc[index * piece + piece // 2 : (index + 1) * piece]
            lanes = lax.broadcasted_iota(jnp.int32, top.shape, 1)
            folded = jnp.where(lanes < half, turn(top), low).astype(jnp.bfloat16)
            packed[block, index] = folded
            here = is_here(block, index, first_row)

            @pl.when(here)
            def _():
                att[landing(first_row)] = folded

            @pl.when(jnp.logical_not(here))
            def _():
                back(block, index, first_row).start()

        return carry

    lax.fori_loop(0, n_sp, visit, 0)

    for sub in range(subs):
        share = (col * device_rows + sub * piece) // rows
        source_share = lax.rem(share + n_sp * share_count - me, share_count)
        for source_col in range(n_tp):
            for pair in range(heads // 2):
                values = []
                for head in (2 * pair, 2 * pair + 1):
                    slot = (source_col * heads + head) * subs + sub
                    source = head * share_count + source_share

                    @pl.when(jnp.logical_not(jnp.logical_and(source == me, source_col == col)))
                    def _():
                        arrived(att.at[slot], back_recv.at[slot])

                    values.append(att[slot].astype(jnp.float32))
                lanes = lax.broadcasted_iota(jnp.int32, values[0].shape, 1)
                top = jnp.where(lanes < half, values[0], turn(values[1]))
                low = jnp.where(lanes < half, turn(values[0]), values[1])
                start = (source_col * heads + 2 * pair) * half
                cols = slice(start, start + width)
                middle = sub * piece + piece // 2
                att_rows[sub * piece : middle, cols] = top.astype(jnp.bfloat16)
                att_rows[middle : (sub + 1) * piece, cols] = low.astype(jnp.bfloat16)

    arrived(wfull.at[sibling], wo_recv.at[sibling])
    for k in range(1, places):
        block = lax.rem(place + k, places) * 2 + 1 - core
        arrived(wfull.at[block], wo_recv.at[block])
    for first in range(0, out_ref.shape[1], COLS):
        w = wfull[:, :, first : first + COLS].reshape(att_rows.shape[1], COLS)
        out_ref[:, first : first + COLS] = jnp.dot(
            att_rows[...], w, preferred_element_type=jnp.float32
        ).astype(jnp.bfloat16)

    for kind in range(2 * places - 1):
        wo_copy(kind).wait_send()
        for part in range(PARTS):
            token_copy(kind, part).wait_send()
    for step in range(1, n_sp):
        q_copy(step).wait_send()
    for share in range(share_count):
        for step in range(1, heads):
            kv_copy(step, share).wait_send()
        for turn_of in range(heads):
            for step in range(1, share_count):
                forward(turn_of, step, share).wait_send()

    def drain(block, carry):
        first_row = lax.rem(my_share + block, share_count) * rows
        for index in range(pieces):
            here = is_here(block, index, first_row)

            @pl.when(jnp.logical_not(here))
            def _():
                back(block, index, first_row).wait_send()

        return carry

    lax.fori_loop(0, n_sp, drain, 0)


def shards(tokens, w_query, w_key, w_value, head_bias, w_out):
    model, local_width = w_query.shape
    heads = head_bias.shape[0]
    width = 2 * (local_width // heads)
    n_sp = lax.axis_size("sp")
    n_tp = lax.axis_size("tp")
    device_rows = tokens.shape[0]
    share_count = n_sp // heads
    rows = device_rows * n_tp // share_count
    piece = min(rows, device_rows)
    pieces = rows // piece
    slots = n_tp * heads * device_rows // piece
    out_width = w_out.shape[1]
    places = n_tp // 2
    kinds = 2 * places - 1

    smem = pl.BlockSpec(memory_space=pltpu.SMEM)
    anywhere = pl.BlockSpec(memory_space=pl.ANY)
    dma = pltpu.SemaphoreType.DMA

    def vmem(*shape):
        return pltpu.VMEM(shape, jnp.bfloat16)

    return pl.pallas_call(
        functools.partial(layer_kernel, n_sp, n_tp, heads),
        out_shape=jax.ShapeDtypeStruct((device_rows, out_width), jnp.bfloat16),
        in_specs=[smem] + [anywhere] * 5,
        out_specs=pl.BlockSpec(memory_space=pltpu.VMEM),
        scratch_shapes=[
            vmem(n_tp, PARTS, device_rows // PARTS, model),
            vmem(3, model, local_width),
            vmem(n_tp, local_width, out_width),
            vmem(heads, share_count, rows, width),
            vmem(heads, share_count, rows // 2, width),
            vmem(n_sp, rows // 2, width),
            vmem(n_sp, share_count, rows, width),
            vmem(n_sp, pieces, piece // 2, width),
            vmem(slots, piece // 2, width),
            vmem(device_rows, n_tp * local_width),
            vmem(CHUNK, CHUNK),
            dma((5,)),
            dma((kinds, PARTS)),
            dma((n_tp, PARTS)),
            dma((kinds,)),
            dma((n_tp,)),
            dma((heads, share_count)),
            dma((heads, share_count, share_count)),
            dma((n_sp, share_count)),
            dma((n_sp,)),
            dma((n_sp,)),
            dma((n_sp, pieces)),
            dma((slots,)),
        ],
        compiler_params=pltpu.CompilerParams(
            collective_id=0, has_side_effects=True, vmem_limit_bytes=60 * 2**20
        ),
        name="layer",
    )(
        head_bias,
        tokens.reshape(PARTS, device_rows // PARTS, model),
        w_query, w_key, w_value, w_out,
    )


def solution(mesh):
    placed = (
        P(("sp", "tp"), None),
        P(None, "tp"),
        P(None, "tp"),
        P(None, "tp"),
        P("tp"),
        P("tp", None),
    )
    return jax.shard_map(
        shards, mesh=mesh, in_specs=placed, out_specs=P(("sp", "tp"), None), check_vma=False
    )
```

```python
import functools
import math

import jax
import jax.numpy as jnp
from jax import lax
from jax.experimental import pallas as pl
from jax.experimental.pallas import tpu as pltpu
from jax.sharding import PartitionSpec as P

MESH = pl.DeviceIdType.MESH
LOG2E = math.log2(math.e)
CHUNK = 256
PARTS = 4
COLS = 512
LOOK = 4
LOG_MAX = 126.0


def layer_kernel(
    n_sp, n_tp, heads, bias_ref, tokens_ref, wq_ref, wk_ref, wv_ref, wo_ref, out_ref,
    tok, wqkv, wfull, kv_own, q_own, q_all, kv_all, packed, att, att_rows, tri,
    load_sem, tok_send, tok_recv, wo_send, wo_recv, kv_send, pass_send, kv_recv, q_send, q_recv,
    back_send, back_recv,
):
    me = lax.axis_index("sp")
    col = lax.axis_index("tp")
    share_count = n_sp // heads
    device_rows = PARTS * tokens_ref.shape[1]
    rows, width = kv_own.shape[2], kv_own.shape[3]
    half = width // 2
    piece = min(rows, device_rows)
    pieces = rows // piece
    subs = device_rows // piece
    chunk_shares = CHUNK // rows
    seg_chunks = share_count * rows // CHUNK
    my_head = me // share_count
    my_share = lax.rem(me, share_count)
    core = lax.rem(col, 2)
    place = col // 2
    places = n_tp // 2
    sibling = place * 2 + 1 - core

    loads = [
        pltpu.make_async_copy(src, dst, load_sem.at[index])
        for index, (src, dst) in enumerate(
            [
                (tokens_ref, tok.at[col]),
                (wq_ref, wqkv.at[0]),
                (wk_ref, wqkv.at[1]),
                (wv_ref, wqkv.at[2]),
                (wo_ref, wfull.at[col]),
            ]
        )
    ]
    for copy in loads:
        copy.start()

    barrier = pltpu.get_barrier_semaphore()
    total = n_sp * n_tp
    flat = me * n_tp + col

    def greet(step, carry):
        other = lax.rem(flat + step, total)
        pl.semaphore_signal(
            barrier, inc=1, device_id=(other // n_tp, lax.rem(other, n_tp)), device_id_type=MESH
        )
        return carry

    lax.fori_loop(1, total, greet, 0)
    key_id = lax.broadcasted_iota(jnp.int32, (CHUNK, CHUNK), 0)
    out_id = lax.broadcasted_iota(jnp.int32, (CHUNK, CHUNK), 1)
    tri[...] = jnp.where(key_id > out_id, 1.0, 0.0).astype(jnp.bfloat16)
    pl.semaphore_wait(barrier, total - 1)

    def same_core(k):
        return lax.rem(place + k, places) * 2 + core

    def arrived(ref, sem):
        pltpu.make_async_copy(ref, ref, sem).wait()

    def token_copy(kind, part):
        if kind < places:
            src, block = tokens_ref.at[part], col
            target = sibling if kind == 0 else same_core(kind)
        else:
            block = same_core(kind - places + 1)
            src, target = tok.at[block, part], sibling
        return pltpu.make_async_remote_copy(
            src_ref=src, dst_ref=tok.at[block, part],
            send_sem=tok_send.at[kind, part], recv_sem=tok_recv.at[block, part],
            device_id=(me, target), device_id_type=MESH,
        )

    def wo_copy(kind):
        if kind < places:
            src, block = wo_ref, col
            target = sibling if kind == 0 else same_core(kind)
        else:
            block = same_core(kind - places + 1)
            src, target = wfull.at[block], sibling
        return pltpu.make_async_remote_copy(
            src_ref=src, dst_ref=wfull.at[block],
            send_sem=wo_send.at[kind], recv_sem=wo_recv.at[block],
            device_id=(me, target), device_id_type=MESH,
        )

    for part in range(PARTS):
        for kind in range(places):
            token_copy(kind, part).start()
    for kind in range(1, places):
        wo_copy(kind).start()

    lane = lax.broadcasted_iota(jnp.int32, (rows, width), 1)
    lane_half = lax.broadcasted_iota(jnp.int32, (rows // 2, width), 1)

    def turn(value):
        return pltpu.roll(value, half, 1)

    def kv_copy(step, share):
        head = lax.rem(my_head + step, heads)
        return pltpu.make_async_remote_copy(
            src_ref=kv_own.at[head, share], dst_ref=kv_all.at[me, share],
            send_sem=kv_send.at[step, share], recv_sem=kv_recv.at[me, share],
            device_id=(head * share_count + my_share, col), device_id_type=MESH,
        )

    def forward(turn_of, step, share):
        block = turn_of * share_count + my_share
        peer = my_head * share_count + lax.rem(my_share + step, share_count)
        return pltpu.make_async_remote_copy(
            src_ref=kv_all.at[block, share], dst_ref=kv_all.at[block, share],
            send_sem=pass_send.at[turn_of, step, share], recv_sem=kv_recv.at[block, share],
            device_id=(peer, col), device_id_type=MESH,
        )

    def relay(block):
        for share in range(share_count):
            arrived(kv_all.at[block, share], kv_recv.at[block, share])
            for step in range(1, share_count):
                forward(block // share_count, step, share).start()

    def share_of(peer):
        return lax.rem(lax.rem(peer, share_count) + me, share_count)

    def q_copy(step):
        peer = lax.rem(me + step, n_sp)
        return pltpu.make_async_remote_copy(
            src_ref=q_own.at[peer // share_count, share_of(peer)], dst_ref=q_all.at[me],
            send_sem=q_send.at[step], recv_sem=q_recv.at[me],
            device_id=(peer, col), device_id_type=MESH,
        )

    def project(group):
        x = tok[pl.ds(group * pieces, pieces)].reshape(subs * rows, tok.shape[3])
        qf = jnp.dot(x, wqkv[0], preferred_element_type=jnp.float32) * (LOG2E * half ** (-0.5))
        kf = jnp.dot(x, wqkv[1], preferred_element_type=jnp.float32)
        vf = jnp.dot(x, wqkv[2], preferred_element_type=jnp.float32)
        for sub in range(subs):
            own = slice(sub * rows, (sub + 1) * rows)
            publish(group * subs + sub, qf[own], kf[own], vf[own])

    def publish(share, qf, kf, vf):
        for pair in range(heads // 2):
            cols = slice(pair * width, (pair + 1) * width)
            kk, vv = kf[:, cols], vf[:, cols]
            top, low = qf[: rows // 2, cols], qf[rows // 2 :, cols]
            kv_own[2 * pair, share] = jnp.where(lane < half, kk, turn(vv)).astype(jnp.bfloat16)
            kv_own[2 * pair + 1, share] = jnp.where(lane < half, turn(kk), vv).astype(jnp.bfloat16)
            q_own[2 * pair, share] = jnp.where(lane_half < half, top, turn(low)).astype(
                jnp.bfloat16
            )
            q_own[2 * pair + 1, share] = jnp.where(lane_half < half, turn(top), low).astype(
                jnp.bfloat16
            )
        for step in range(1, heads):
            kv_copy(step, share).start()
        kv_all[me, share] = kv_own[my_head, share]
        for step in range(1, share_count):
            forward(my_head, step, share).start()
        for step in range(1, n_sp):

            @pl.when(share_of(lax.rem(me + step, n_sp)) == share)
            def _():
                q_copy(step).start()

        @pl.when(share_of(me) == share)
        def _():
            q_all[me] = q_own[my_head, share]

    for copy in loads:
        copy.wait()
    own_group = col // pieces
    groups = n_tp // pieces
    if pieces > 1:
        for part in range(PARTS):
            arrived(tok.at[sibling, part], tok_recv.at[sibling, part])
        project(own_group)
    for part in range(PARTS):
        for k in range(1, places):
            block = same_core(k)
            arrived(tok.at[block, part], tok_recv.at[block, part])
            token_copy(places + k - 1, part).start()
    for part in range(PARTS):
        if pieces == 1:
            arrived(tok.at[sibling, part], tok_recv.at[sibling, part])
        for k in range(1, places):
            block = lax.rem(place + k, places) * 2 + 1 - core
            arrived(tok.at[block, part], tok_recv.at[block, part])

    def project_next(step, carry):
        project(lax.rem(own_group + step, groups))
        return carry

    lax.fori_loop(1 if pieces > 1 else 0, groups, project_next, 0)

    wo_copy(0).start()
    bias = bias_ref[my_head] * LOG2E

    def logs(q, keys):
        scores = lax.dot_general(
            q, keys, (((1,), (1,)), ((), ())), preferred_element_type=jnp.float32
        )
        z = scores + bias
        lose = jnp.maximum(
            jnp.log(1.0 + jnp.exp2(jnp.minimum(z, LOG_MAX))) * LOG2E, z
        )
        return z - lose, lose

    def tails(lose):
        lose = lose.astype(jnp.bfloat16)
        tail = jnp.dot(lose, tri[...], preferred_element_type=jnp.float32)
        return tail, tail[:, 0:1] + lose[:, 0:1].astype(jnp.float32)

    def chunk_keys(index):
        block, inner = index // seg_chunks, lax.rem(index, seg_chunks)
        return kv_all[block, pl.ds(inner * chunk_shares, chunk_shares)].reshape(CHUNK, width)

    def weigh(log_take, tail, later, keys):
        weight = jnp.exp2(log_take - tail).astype(jnp.bfloat16)
        return jnp.exp2(-later) * jnp.dot(weight, keys, preferred_element_type=jnp.float32)

    def landing(first_row):
        return (col * heads + my_head) * subs + lax.rem(first_row // piece, subs)

    def is_here(block, index, first_row):
        return jnp.logical_and(block == me, (first_row + index * piece) // device_rows == col)

    def back(block, index, first_row):
        owner = (first_row + index * piece) // device_rows
        slot = landing(first_row)
        return pltpu.make_async_remote_copy(
            src_ref=packed.at[block, index], dst_ref=att.at[slot],
            send_sem=back_send.at[block, index], recv_sem=back_recv.at[slot],
            device_id=(block, owner), device_id_type=MESH,
        )

    def relayed(block):
        return jnp.logical_and(lax.rem(block, share_count) == my_share, block != me)

    for block in range(LOOK):

        @pl.when(relayed(block))
        def _():
            relay(block)

    def visit(block, carry):
        ahead = block + LOOK

        @pl.when(jnp.logical_and(ahead < n_sp, relayed(ahead)))
        def _():
            relay(ahead)

        @pl.when(lax.rem(block, share_count) != my_share)
        def _():
            for share in range(share_count):
                arrived(kv_all.at[block, share], kv_recv.at[block, share])

        @pl.when(block != me)
        def _():
            arrived(q_all.at[block], q_recv.at[block])

        @pl.when(block == n_sp - 1)
        def _():
            for k in range(1, places):
                arrived(wfull.at[same_core(k)], wo_recv.at[same_core(k)])
                wo_copy(places + k - 1).start()

        pair = q_all[block].astype(jnp.float32)
        low = jnp.where(lane_half < half, pair, 0.0)
        high = jnp.where(lane_half < half, turn(pair), 0.0)
        q = jnp.concatenate([low, high], axis=0).astype(jnp.bfloat16)
        first_row = lax.rem(my_share + block, share_count) * rows
        diagonal = first_row // CHUNK
        q_pos = first_row + lax.broadcasted_iota(jnp.int32, (rows, CHUNK), 0)
        k_pos = diagonal * CHUNK + lax.broadcasted_iota(jnp.int32, (rows, CHUNK), 1)
        live = k_pos < q_pos

        keys = chunk_keys(block * seg_chunks + diagonal)
        log_take, keep = logs(q, keys)
        tail, later = tails(jnp.where(live, keep, 0.0))
        weight = jnp.where(live, jnp.exp2(log_take - tail), 0.0).astype(jnp.bfloat16)
        acc = jnp.dot(weight, keys, preferred_element_type=jnp.float32)

        def single(step, state):
            acc, later = state
            keys = chunk_keys(block * seg_chunks + diagonal - 1 - step)
            log_take, keep = logs(q, keys)
            tail, whole = tails(keep)
            return acc + weigh(log_take, tail, later, keys), later + whole

        def segment(step, state):
            acc, later = state
            first = (block - 1 - step) * seg_chunks
            keys = [chunk_keys(first + index) for index in reversed(range(seg_chunks))]
            terms = [logs(q, part) for part in keys]
            ends = [tails(keep) for _, keep in terms]
            for part, (log_take, _), (tail, whole) in zip(keys, terms, ends):
                acc = acc + weigh(log_take, tail, later, part)
                later = later + whole
            return acc, later

        state = lax.fori_loop(0, diagonal, single, (acc, later))
        acc, _ = lax.fori_loop(0, block, segment, state)
        for index in range(pieces):
            top = acc[index * piece : index * piece + piece // 2]
            low = acc[index * piece + piece // 2 : (index + 1) * piece]
            lanes = lax.broadcasted_iota(jnp.int32, top.shape, 1)
            folded = jnp.where(lanes < half, turn(top), low).astype(jnp.bfloat16)
            packed[block, index] = folded
            here = is_here(block, index, first_row)

            @pl.when(here)
            def _():
                att[landing(first_row)] = folded

            @pl.when(jnp.logical_not(here))
            def _():
                back(block, index, first_row).start()

        return carry

    lax.fori_loop(0, n_sp, visit, 0)

    for sub in range(subs):
        share = (col * device_rows + sub * piece) // rows
        source_share = lax.rem(share + n_sp * share_count - me, share_count)
        for source_col in range(n_tp):
            for pair in range(heads // 2):
                values = []
                for head in (2 * pair, 2 * pair + 1):
                    slot = (source_col * heads + head) * subs + sub
                    source = head * share_count + source_share

                    @pl.when(jnp.logical_not(jnp.logical_and(source == me, source_col == col)))
                    def _():
                        arrived(att.at[slot], back_recv.at[slot])

                    values.append(att[slot].astype(jnp.float32))
                lanes = lax.broadcasted_iota(jnp.int32, values[0].shape, 1)
                top = jnp.where(lanes < half, values[0], turn(values[1]))
                low = jnp.where(lanes < half, turn(values[0]), values[1])
                start = (source_col * heads + 2 * pair) * half
                cols = slice(start, start + width)
                middle = sub * piece + piece // 2
                att_rows[sub * piece : middle, cols] = top.astype(jnp.bfloat16)
                att_rows[middle : (sub + 1) * piece, cols] = low.astype(jnp.bfloat16)

    arrived(wfull.at[sibling], wo_recv.at[sibling])
    for k in range(1, places):
        block = lax.rem(place + k, places) * 2 + 1 - core
        arrived(wfull.at[block], wo_recv.at[block])
    for first in range(0, out_ref.shape[1], COLS):
        w = wfull[:, :, first : first + COLS].reshape(att_rows.shape[1], COLS)
        out_ref[:, first : first + COLS] = jnp.dot(
            att_rows[...], w, preferred_element_type=jnp.float32
        ).astype(jnp.bfloat16)

    for kind in range(2 * places - 1):
        wo_copy(kind).wait_send()
        for part in range(PARTS):
            token_copy(kind, part).wait_send()
    for step in range(1, n_sp):
        q_copy(step).wait_send()
    for share in range(share_count):
        for step in range(1, heads):
            kv_copy(step, share).wait_send()
        for turn_of in range(heads):
            for step in range(1, share_count):
                forward(turn_of, step, share).wait_send()

    def drain(block, carry):
        first_row = lax.rem(my_share + block, share_count) * rows
        for index in range(pieces):
            here = is_here(block, index, first_row)

            @pl.when(jnp.logical_not(here))
            def _():
                back(block, index, first_row).wait_send()

        return carry

    lax.fori_loop(0, n_sp, drain, 0)


def shards(tokens, w_query, w_key, w_value, head_bias, w_out):
    model, local_width = w_query.shape
    heads = head_bias.shape[0]
    width = 2 * (local_width // heads)
    n_sp = lax.axis_size("sp")
    n_tp = lax.axis_size("tp")
    device_rows = tokens.shape[0]
    share_count = n_sp // heads
    rows = device_rows * n_tp // share_count
    piece = min(rows, device_rows)
    pieces = rows // piece
    slots = n_tp * heads * device_rows // piece
    out_width = w_out.shape[1]
    places = n_tp // 2
    kinds = 2 * places - 1

    smem = pl.BlockSpec(memory_space=pltpu.SMEM)
    anywhere = pl.BlockSpec(memory_space=pl.ANY)
    dma = pltpu.SemaphoreType.DMA

    def vmem(*shape):
        return pltpu.VMEM(shape, jnp.bfloat16)

    return pl.pallas_call(
        functools.partial(layer_kernel, n_sp, n_tp, heads),
        out_shape=jax.ShapeDtypeStruct((device_rows, out_width), jnp.bfloat16),
        in_specs=[smem] + [anywhere] * 5,
        out_specs=pl.BlockSpec(memory_space=pltpu.VMEM),
        scratch_shapes=[
            vmem(n_tp, PARTS, device_rows // PARTS, model),
            vmem(3, model, local_width),
            vmem(n_tp, local_width, out_width),
            vmem(heads, share_count, rows, width),
            vmem(heads, share_count, rows // 2, width),
            vmem(n_sp, rows // 2, width),
            vmem(n_sp, share_count, rows, width),
            vmem(n_sp, pieces, piece // 2, width),
            vmem(slots, piece // 2, width),
            vmem(device_rows, n_tp * local_width),
            vmem(CHUNK, CHUNK),
            dma((5,)),
            dma((kinds, PARTS)),
            dma((n_tp, PARTS)),
            dma((kinds,)),
            dma((n_tp,)),
            dma((heads, share_count)),
            dma((heads, share_count, share_count)),
            dma((n_sp, share_count)),
            dma((n_sp,)),
            dma((n_sp,)),
            dma((n_sp, pieces)),
            dma((slots,)),
        ],
        compiler_params=pltpu.CompilerParams(
            collective_id=0, has_side_effects=True, vmem_limit_bytes=60 * 2**20
        ),
        name="layer",
    )(
        head_bias,
        tokens.reshape(PARTS, device_rows // PARTS, model),
        w_query, w_key, w_value, w_out,
    )


def solution(mesh):
    placed = (
        P(("sp", "tp"), None),
        P(None, "tp"),
        P(None, "tp"),
        P(None, "tp"),
        P("tp"),
        P("tp", None),
    )
    return jax.shard_map(
        shards, mesh=mesh, in_specs=placed, out_specs=P(("sp", "tp"), None), check_vma=False
    )
```
